32 devices in a mesh: tp: 8 (over z, x), dp: 4 (over y, core).
Axes of the slice: x: 2, y: 2, z: 4, core: 2. Of those that a mesh axis runs over, the one named last changes fastest.
Arguments:
- stream_in: bfloat16 [256, 4096], P('tp', 'dp'), may hold values from -21 to 21
- hidden_state: float32 [2, 256, 4096], P(None, 'dp', 'tp'), may hold values from -6 to 6
- convolution_window_state: bfloat16 [2, 256, 3, 4096], P(None, 'dp', None, 'tp'), may hold values from -6 to 6
- norm_gain: float32 [2, 4096], P(None, 'dp'), may hold values from 0.1 to 1.9
- path_weight: bfloat16 [2, 4096, 4096], P(None, 'dp', 'tp'), may hold values from -0.09375 to 0.09375
- output_gate_weight: bfloat16 [2, 4096, 4096], P(None, 'dp', 'tp'), may hold values from -0.09375 to 0.09375
- conv_taps: float32 [2, 4, 4096], P(None, None, 'tp'), may hold values from -3 to 3
- recur_map: float32 [2, 64, 64, 64], P(None, 'tp'), may hold values from -0.75 to 0.75
- input_map: float32 [2, 64, 64, 64], P(None, 'tp'), may hold values from -0.75 to 0.75
- decay_logit: float32 [2, 4096], P(None, 'tp'), may hold values from 1 to 6
- out_weight: bfloat16 [2, 4096, 4096], P(None, 'tp', 'dp'), may hold values from -0.09375 to 0.09375
Outputs:
- stream_out: bfloat16 [256, 4096], P('tp', 'dp')
- hidden_next: float32 [2, 256, 4096], P(None, 'dp', 'tp')
- conv_next: bfloat16 [2, 256, 3, 4096], P(None, 'dp', None, 'tp')
The draws below stay inside these ranges and needn't reach their ends.
All inputs are finite; a program needn't handle non-finite values.
Results may differ from the reference program's by a relative error of at most 0.019.
Values may be sent and summed in bfloat16 or wider, within the bound.
A program may use at most 64 MiB of HBM per device.

```python
import jax
import jax.numpy as jnp
from jax import lax

D = 4096
R = 4096
BLOCK_W = 64
NBLK = 64
LAYERS = 2
TAPS = 4
BATCH = 256
N_DP = 4


def draw_stream_in(key, part):
    first, second = jax.random.split(key, 2)
    groups = D // 64
    group_scale = jnp.exp(jax.random.uniform(first, (groups,), jnp.float32, jnp.log(0.3), jnp.log(3.0)))
    column_scale = jnp.repeat(group_scale, 64)
    values = jnp.clip(jax.random.normal(second, (BATCH, D), jnp.float32), -4.0, 4.0)
    return (values * column_scale[None, :]).astype(jnp.bfloat16)


def level_of(rng, dims, cuts, low, largest):
    loudness = 1.0
    for axis_at, shards_of in cuts:
        steps = jax.random.uniform(jax.random.fold_in(jax.random.fold_in(rng, 6), axis_at), (shards_of,), jnp.float32, low / len(cuts), largest / len(cuts))
        loudness = loudness * jnp.repeat(jnp.exp(steps), dims[axis_at] // shards_of).reshape((-1,) + (1,) * (len(dims) - 1 - axis_at))
    return loudness


def scatter_about(rng, extent, scale, most, shards=(), dtype=jnp.bfloat16):
    factor_of = level_of(rng, extent, shards, -0.22, 0.18) if shards else 1.0
    drawn = jax.random.normal(rng, extent, jnp.float32) * scale * factor_of
    return jnp.minimum(jnp.maximum(drawn, -most), most).astype(dtype)


def setup_inputs(seed: int = 0) -> dict:
    streams_of = jax.random.split(jax.random.key(seed), 12)
    return {
        "stream_in": draw_stream_in(jax.random.fold_in(streams_of[11], 71), 0),
        "hidden_state": scatter_about(streams_of[1], (LAYERS, BATCH, R), 1.0, 6.0, ((1, 4), (2, 8)), jnp.float32),
        "convolution_window_state": scatter_about(streams_of[2], (LAYERS, BATCH, TAPS - 1, R), 1.0, 6.0, ((1, 4), (3, 8))),
        "norm_gain": jnp.clip(1.0 + 0.18 * jax.random.normal(streams_of[3], (LAYERS, D), jnp.float32), 0.1, 1.9),
        "path_weight": scatter_about(streams_of[4], (LAYERS, D, R), D ** -0.5, 0.09375, ((1, 4), (2, 8))),
        "output_gate_weight": scatter_about(streams_of[5], (LAYERS, D, R), D ** -0.5, 0.09375, ((1, 4), (2, 8))),
        "conv_taps": scatter_about(streams_of[6], (LAYERS, TAPS, R), 0.5, 3.0, ((2, 8),), jnp.float32),
        "recur_map": scatter_about(streams_of[7], (LAYERS, NBLK, BLOCK_W, BLOCK_W), BLOCK_W ** -0.5, 0.75, ((1, 8),), jnp.float32),
        "input_map": scatter_about(streams_of[8], (LAYERS, NBLK, BLOCK_W, BLOCK_W), BLOCK_W ** -0.5, 0.75, ((1, 8),), jnp.float32),
        "decay_logit": jnp.clip(1.0 + 5.0 * jax.random.uniform(streams_of[9], (LAYERS, R), jnp.float32) ** level_of(streams_of[9], (LAYERS, R), ((1, 8),), -0.2, 0.2), 1.0, 6.0),
        "out_weight": scatter_about(streams_of[10], (LAYERS, R, D), R ** -0.5, 0.09375, ((1, 8), (2, 4))),
    }


EPS = 1e-06

def one_block(stream, hidden, buffer, gain, path_w, gate_branch_matrix, taps, recur_w, input_matrix, logit, out_w):
    batch = stream.shape[0]
    streamf = stream.astype(jnp.float32)
    sumsq = lax.optimization_barrier(jnp.sum(streamf * streamf, axis=1))
    normed = (streamf * lax.rsqrt(sumsq / D + EPS)[:, None] * gain[None, :]).astype(jnp.bfloat16)
    block_list = normed.astype(jnp.float32).reshape(batch, N_DP, D // N_DP)

    def summed(weight):
        weight_block_list = weight.astype(jnp.float32).reshape(N_DP, D // N_DP, R)
        piece_list = jnp.einsum('yiq,iqx->iyx', block_list, weight_block_list).astype(jnp.bfloat16)
        piece_list = lax.optimization_barrier(piece_list).astype(jnp.float32)
        return lax.optimization_barrier(jnp.sum(piece_list, axis=0)).astype(jnp.bfloat16)
    zpath = summed(path_w)
    zgate = summed(gate_branch_matrix)
    conv = zpath.astype(jnp.float32) * taps[TAPS - 1][None, :]
    for j in range(TAPS - 1):
        conv = conv + buffer[:, j].astype(jnp.float32) * taps[j][None, :]
    new_buffer = jnp.concatenate([buffer[:, 1:], zpath[:, None, :]], axis=1)
    cblocks = conv.reshape(batch, NBLK, BLOCK_W)
    rgate = jax.nn.sigmoid(jnp.einsum('bnc,ncd->bnd', cblocks, recur_w, precision=lax.Precision.HIGHEST).reshape(batch, R))
    igate = jax.nn.sigmoid(jnp.einsum('bnc,ncd->bnd', cblocks, input_matrix, precision=lax.Precision.HIGHEST).reshape(batch, R))
    loga = 8.0 * rgate * jax.nn.log_sigmoid(logit)[None, :]
    new_hidden = jnp.exp(loga) * hidden + jnp.sqrt(-jnp.expm1(2.0 * loga)) * (igate * conv)
    mixed = (new_hidden * jax.nn.gelu(zgate.astype(jnp.float32))).astype(jnp.bfloat16)
    update = jnp.dot(mixed, out_w, preferred_element_type=jnp.float32)
    return ((streamf + update).astype(jnp.bfloat16), new_hidden, new_buffer)

def reference(stream_in, hidden_state, convolution_window_state, norm_gain, path_weight, output_gate_weight, conv_taps, recur_map, input_map, decay_logit, out_weight):
    stream = stream_in
    hiddens = []
    buffers = []
    for layer in range(LAYERS):
        stream, new_hidden, new_buffer = one_block(stream, hidden_state[layer], convolution_window_state[layer], norm_gain[layer], path_weight[layer], output_gate_weight[layer], conv_taps[layer], recur_map[layer], input_map[layer], decay_logit[layer], out_weight[layer])
        hiddens.append(new_hidden)
        buffers.append(new_buffer)
    return (stream, jnp.stack(hiddens), jnp.stack(buffers))
```

```python
import functools

import jax
import jax.numpy as jnp
from jax import lax
from jax.experimental import pallas as pl
from jax.experimental.pallas import tpu as pltpu
from jax.sharding import PartitionSpec as P

EPS = 1e-06
MESH = pl.DeviceIdType.MESH
LANES = 128
F32 = jnp.float32
BF16 = jnp.bfloat16


def partner(index, step, count):
    if count & (count - 1):
        raise ValueError(count)
    out = index
    bit = 1
    while bit < count:
        if step & bit:
            out = out + bit - 2 * bit * ((index // bit) % 2)
        bit *= 2
    return out


def pack_col(col):
    high = col.astype(BF16).astype(F32)
    low = col - high
    lane = lax.broadcasted_iota(jnp.int32, (col.shape[0], LANES), 1)
    return jnp.where(lane < LANES // 2, high, low).astype(BF16)


def unpack_col(lanes):
    return lanes[:, 0:1] + lanes[:, LANES // 2 : LANES // 2 + 1]


def step_kernel(
    sizes,
    stream, hidden_hbm, convpart_hbm, gain, path_hbm, gate_hbm, taps, rmap_hbm, imap_hbm, logit, outw_hbm,
    stream_out, hidden_out, zpath_out,
    xg, part, core_in, y_send, y_in, mix, upd, x_in, z_send, z_in,
    wpath, wgate, wout, hid, convp, rmap, imap, diag,
    load_sem, load_small, ag_s, ag_r, fw_s, fw_r, b1_s, b1_r, b2_s, b2_r,
    c1_s, c1_r, c2_s, c2_r, d1_s, d1_r, d2_s, d2_r,
):
    layers, nz, nx, ny, nc, model = sizes
    tp = lax.axis_index("tp")
    dp = lax.axis_index("dp")
    z, x = tp // nx, tp % nx
    y, c = dp // nc, dp % nc
    rows, cols = stream.shape
    chans = wpath.shape[2]
    per_z = mix.shape[1] // nz
    chunk = mix.shape[2]

    def on_tp(zz, xx):
        return {"tp": zz * nx + xx, "dp": dp}

    def on_dp(yy, cc):
        return {"tp": tp, "dp": yy * nc + cc}

    loads = {}

    def load(name, layer, src, dst, sem):
        copy = pltpu.make_async_copy(src.at[layer], dst.at[layer], sem)
        copy.start()
        loads[name, layer] = copy

    peers = (
        [on_tp(partner(z, k, nz), x) for k in range(1, nz)]
        + [on_tp(z, partner(x, k, nx)) for k in range(1, nx)]
        + [on_dp(partner(y, k, ny), c) for k in range(1, ny)]
        + [on_dp(y, partner(c, k, nc)) for k in range(1, nc)]
    )
    barrier = pltpu.get_barrier_semaphore()
    for peer in peers:
        pl.semaphore_signal(barrier, inc=1, device_id=peer, device_id_type=MESH)
    xg[0, tp] = stream[...]
    load("path", 0, path_hbm, wpath, load_sem.at[0, 0])
    load("gate", 0, gate_hbm, wgate, load_sem.at[0, 1])
    for layer in range(layers):
        load("rmap", layer, rmap_hbm, rmap, load_small.at[layer, 0])
        load("imap", layer, imap_hbm, imap, load_small.at[layer, 1])
    pl.semaphore_wait(barrier, len(peers))

    sends = []

    def send(src, dst, ssem, rsem, peer):
        copy = pltpu.make_async_remote_copy(
            src_ref=src, dst_ref=dst, send_sem=ssem, recv_sem=rsem, device_id=peer, device_id_type=MESH
        )
        copy.start()
        sends.append(copy)

    def arrived(dst, ssem, rsem, peer):
        pltpu.make_async_remote_copy(
            src_ref=dst, dst_ref=dst, send_sem=ssem, recv_sem=rsem, device_id=peer, device_id_type=MESH
        ).wait_recv()

    def gather_start(layer):
        own = xg.at[layer, tp]
        source = stream if layer == 0 else own
        for k in range(1, nz):
            send(source, own, ag_s.at[layer, k], ag_r.at[layer, k], on_tp(partner(z, k, nz), x))
        for j in range(1, nx):
            send(source, own, fw_s.at[layer, 0, j], fw_r.at[layer, 0, j], on_tp(z, partner(x, j, nx)))

    def project(layer, zz):
        block = xg[layer, pl.ds(zz * nx, nx)].reshape(nx * rows, cols).astype(F32)
        scaled = (block * gain[layer : layer + 1, :]).astype(BF16)
        square = jnp.sum(block * block, axis=1, keepdims=True)
        shape = (per_z, chunk)
        here = pl.ds(zz * per_z, per_z)
        part[layer, here, :, 0:chans] = (
            jnp.dot(scaled, wpath[layer], preferred_element_type=F32).astype(BF16).reshape(*shape, chans)
        )
        part[layer, here, :, chans : 2 * chans] = (
            jnp.dot(scaled, wgate[layer], preferred_element_type=F32).astype(BF16).reshape(*shape, chans)
        )
        part[layer, here, :, 2 * chans :] = pack_col(square).reshape(*shape, LANES)

    def gather_and_project(layer):
        for k in range(nz):
            zz = partner(z, k, nz)
            if k:
                own = xg.at[layer, zz * nx + x]
                arrived(own, ag_s.at[layer, k], ag_r.at[layer, k], on_tp(zz, x))
                for j in range(1, nx):
                    send(own, own, fw_s.at[layer, k, j], fw_r.at[layer, k, j], on_tp(z, partner(x, j, nx)))
            if k == 0:
                loads["path", layer].wait()
                loads["gate", layer].wait()
            else:
                finish_block(layer, k - 1)
        finish_block(layer, nz - 1)

    def finish_block(layer, k):
        zz = partner(z, k, nz)
        for j in range(1, nx):
            xx = partner(x, j, nx)
            arrived(xg.at[layer, zz * nx + xx], fw_s.at[layer, k, j], fw_r.at[layer, k, j], on_tp(z, xx))
        project(layer, zz)

    def reduce_rows(layer):
        order = list(range(1, ny)) + [0]
        for k in order:
            yy = partner(y, k, ny)
            for j in range(1, nc):
                cc = partner(c, j, nc)
                send(
                    part.at[layer, yy * nc + cc], core_in.at[layer, j, k],
                    b1_s.at[layer, j, k], b1_r.at[layer, j, k], on_dp(y, cc),
                )
        total = None
        for k in order:
            yy = partner(y, k, ny)
            both = part[layer, yy * nc + c].astype(F32)
            extra = None
            for j in range(1, nc):
                arrived(
                    core_in.at[layer, j, k], b1_s.at[layer, j, k], b1_r.at[layer, j, k],
                    on_dp(y, partner(c, j, nc)),
                )
                both = both + core_in[layer, j, k].astype(F32)
            if k:
                y_send[layer, k, :, 0 : 2 * chans] = both[:, : 2 * chans].astype(BF16)
                y_send[layer, k, :, 2 * chans :] = pack_col(unpack_col(both[:, 2 * chans :]))
                send(y_send.at[layer, k], y_in.at[layer, k], b2_s.at[layer, k], b2_r.at[layer, k], on_dp(yy, c))
            else:
                total = both
        for k in range(1, ny):
            arrived(y_in.at[layer, k], b2_s.at[layer, k], b2_r.at[layer, k], on_dp(partner(y, k, ny), c))
            total = total + y_in[layer, k].astype(F32)
        return total

    def recur(layer, total):
        loads["hidden", layer].wait()
        loads["convpart", layer].wait()
        scale = lax.rsqrt(unpack_col(total[:, 2 * chans :]) / model + EPS)
        zpath = (total[:, :chans] * scale).astype(BF16)
        zgate = (total[:, chans : 2 * chans] * scale).astype(BF16).astype(F32)
        zpath_out[layer] = zpath
        last = taps.shape[1] - 1
        conv = convp[layer] + zpath.astype(F32) * taps[layer, last : last + 1, :]
        keep = jax.nn.log_sigmoid(logit[layer : layer + 1, :]) * 8.0
        gated = 0.5 * zgate * (1.0 + jnp.tanh(0.7978845608028654 * (zgate + 0.044715 * zgate * zgate * zgate)))
        wide = diag.shape[2]
        for p in range(diag.shape[1]):
            at = slice(p * wide, (p + 1) * wide)
            cb = conv[:, at]
            both = jnp.dot(cb, diag[layer, p], preferred_element_type=F32, precision=lax.Precision.HIGHEST)
            rgate = jax.nn.sigmoid(both[:, :wide])
            igate = jax.nn.sigmoid(both[:, wide:])
            loga = rgate * keep[:, at]
            decay = jnp.exp(loga)
            new = decay * hid[layer, :, at] + jnp.sqrt(-jnp.tanh(loga) * (1.0 + decay * decay)) * (igate * cb)
            hidden_out[layer, :, at] = new
            mix[layer, dp, :, at] = (new * gated[:, at]).astype(BF16)

    def share_and_emit(layer):
        own = mix.at[layer, dp]
        for k in range(1, ny):
            send(own, own, c1_s.at[layer, k], c1_r.at[layer, k], on_dp(partner(y, k, ny), c))
        for j in range(1, nc):
            send(own, own, c2_s.at[layer, 0, j], c2_r.at[layer, 0, j], on_dp(y, partner(c, j, nc)))
        loads["outw", layer].wait()
        if per_z == 1:
            emit(layer, dp)
        later = []
        for k in range(ny):
            yy = partner(y, k, ny)
            if k:
                theirs = mix.at[layer, yy * nc + c]
                arrived(theirs, c1_s.at[layer, k], c1_r.at[layer, k], on_dp(yy, c))
                for j in range(1, nc):
                    send(theirs, theirs, c2_s.at[layer, k, j], c2_r.at[layer, k, j], on_dp(y, partner(c, j, nc)))
                if per_z == 1:
                    emit(layer, yy * nc + c)
            for j in range(1, nc):
                cc = partner(c, j, nc)
                arrived(
                    mix.at[layer, yy * nc + cc], c2_s.at[layer, k, j], c2_r.at[layer, k, j], on_dp(y, cc)
                )
                if per_z == 1:
                    emit(layer, yy * nc + cc)
        if per_z != 1:
            for zz in range(nz):
                emit(layer, zz)

    def emit(layer, zz):
        block = mix[layer, pl.ds(zz * per_z, per_z)].reshape(per_z * chunk, chans)
        upd[layer, pl.ds(zz * nx, nx)] = (
            jnp.dot(block, wout[layer], preferred_element_type=F32).astype(BF16).reshape(nx, rows, cols)
        )
        for j in range(1, nx):
            xx = partner(x, j, nx)
            send(
                upd.at[layer, zz * nx + xx], x_in.at[layer, j, zz],
                d1_s.at[layer, j, zz], d1_r.at[layer, j, zz], on_tp(z, xx),
            )

    def reduce_stream(layer):
        total = None
        for k in list(range(1, nz)) + [0]:
            zz = partner(z, k, nz)
            both = upd[layer, zz * nx + x].astype(F32)
            for j in range(1, nx):
                arrived(
                    x_in.at[layer, j, zz], d1_s.at[layer, j, zz], d1_r.at[layer, j, zz], on_tp(z, partner(x, j, nx))
                )
                both = both + x_in[layer, j, zz].astype(F32)
            if k:
                z_send[layer, k] = both.astype(BF16)
                send(z_send.at[layer, k], z_in.at[layer, k], d2_s.at[layer, k], d2_r.at[layer, k], on_tp(zz, x))
            else:
                total = both
        for k in range(1, nz):
            arrived(z_in.at[layer, k], d2_s.at[layer, k], d2_r.at[layer, k], on_tp(partner(z, k, nz), x))
            total = total + z_in[layer, k].astype(F32)
        return (xg[layer, tp].astype(F32) + total).astype(BF16)

    gather_start(0)
    for layer in range(layers):
        load("hidden", layer, hidden_hbm, hid, load_sem.at[layer, 2])
        load("convpart", layer, convpart_hbm, convp, load_sem.at[layer, 3])
        load("outw", layer, outw_hbm, wout, load_sem.at[layer, 4])
        if layer:
            load("path", layer, path_hbm, wpath, load_sem.at[layer, 0])
            load("gate", layer, gate_hbm, wgate, load_sem.at[layer, 1])

    width = rmap.shape[2]
    row = lax.broadcasted_iota(jnp.int32, (width, 2 * width), 0)
    col = lax.broadcasted_iota(jnp.int32, (width, 2 * width), 1)
    place = [jnp.where(col == row + half * width, 1.0, 0.0).astype(F32) for half in range(2)]
    for layer in range(layers):
        loads["rmap", layer].wait()
        loads["imap", layer].wait()
        for p in range(diag.shape[1]):
            for half in range(2):
                for which, maps in enumerate((rmap, imap)):
                    diag[
                        layer, p, half * width : (half + 1) * width, which * 2 * width : (which + 1) * 2 * width
                    ] = jnp.dot(
                        maps[layer, 2 * p + half], place[half],
                        preferred_element_type=F32, precision=lax.Precision.HIGHEST,
                    )

    for layer in range(layers):
        gather_and_project(layer)
        recur(layer, reduce_rows(layer))
        share_and_emit(layer)
        new = reduce_stream(layer)
        if layer + 1 < layers:
            xg[layer + 1, tp] = new
            gather_start(layer + 1)
        else:
            stream_out[...] = new
    for copy in sends:
        copy.wait_send()


def per_device(
    grid,
    stream_in, hidden_state, window, norm_gain, path_weight, output_gate_weight,
    conv_taps, recur_map, input_map, decay_logit, out_weight,
):
    nz, nx, ny, nc = grid
    rows, cols = stream_in.shape
    layers, chunk, chans = hidden_state.shape
    tp, dp = nz * nx, ny * nc
    width = recur_map.shape[2]
    blocks = recur_map.shape[1]
    taps = conv_taps.shape[1]
    convpart = sum(window[:, :, j].astype(F32) * conv_taps[:, j][:, None, :] for j in range(taps - 1))
    wide = 2 * chans + LANES
    vm = pl.BlockSpec(memory_space=pltpu.VMEM)
    hbm = pl.BlockSpec(memory_space=pl.ANY)
    dma = pltpu.SemaphoreType.DMA
    stream_out, hidden_next, zpath = pl.pallas_call(
        functools.partial(step_kernel, (layers, nz, nx, ny, nc, cols * dp)),
        out_shape=(
            jax.ShapeDtypeStruct((rows, cols), BF16),
            jax.ShapeDtypeStruct((layers, chunk, chans), F32),
            jax.ShapeDtypeStruct((layers, chunk, chans), BF16),
        ),
        in_specs=[vm, hbm, hbm, vm, hbm, hbm, vm, hbm, hbm, vm, hbm],
        out_specs=(vm, vm, vm),
        scratch_shapes=[
            pltpu.VMEM((layers, tp, rows, cols), BF16),
            pltpu.VMEM((layers, dp, chunk, wide), BF16),
            pltpu.VMEM((layers, nc, ny, chunk, wide), BF16),
            pltpu.VMEM((layers, ny, chunk, wide), BF16),
            pltpu.VMEM((layers, ny, chunk, wide), BF16),
            pltpu.VMEM((layers, dp, chunk, chans), BF16),
            pltpu.VMEM((layers, tp, rows, cols), BF16),
            pltpu.VMEM((layers, nx, nz, rows, cols), BF16),
            pltpu.VMEM((layers, nz, rows, cols), BF16),
            pltpu.VMEM((layers, nz, rows, cols), BF16),
            pltpu.VMEM((layers, cols, chans), BF16),
            pltpu.VMEM((layers, cols, chans), BF16),
            pltpu.VMEM((layers, chans, cols), BF16),
            pltpu.VMEM((layers, chunk, chans), F32),
            pltpu.VMEM((layers, chunk, chans), F32),
            pltpu.VMEM((layers, blocks, width, width), F32),
            pltpu.VMEM((layers, blocks, width, width), F32),
            pltpu.VMEM((layers, blocks // 2, 2 * width, 4 * width), F32),
            dma((layers, 5)), dma((layers, 2)),
            dma((layers, nz)), dma((layers, nz)), dma((layers, nz, nx)), dma((layers, nz, nx)),
            dma((layers, nc, ny)), dma((layers, nc, ny)), dma((layers, ny)), dma((layers, ny)),
            dma((layers, ny)), dma((layers, ny)), dma((layers, ny, nc)), dma((layers, ny, nc)),
            dma((layers, nx, nz)), dma((layers, nx, nz)), dma((layers, nz)), dma((layers, nz)),
        ],
        compiler_params=pltpu.CompilerParams(
            collective_id=0, has_side_effects=True, vmem_limit_bytes=48 * 1024 * 1024
        ),
    )(
        stream_in, hidden_state, convpart, norm_gain, path_weight, output_gate_weight,
        conv_taps, recur_map, input_map, decay_logit, out_weight,
    )
    return stream_out, hidden_next, jnp.concatenate([window[:, :, 1:], zpath[:, :, None]], axis=2)


def physical(mesh):
    first = mesh.devices.flat[0]
    tp, dp = mesh.shape["tp"], mesh.shape["dp"]
    if getattr(first, "coords", None) is None:
        nx, nc = 2, 2
    else:
        nx = len({d.coords[0] for d in mesh.devices.flat})
        nc = len({d.core_on_chip for d in mesh.devices.flat})
    return tp // nx, nx, dp // nc, nc


def solution(mesh):
    placed = (
        P("tp", "dp"),
        P(None, "dp", "tp"),
        P(None, "dp", None, "tp"),
        P(None, "dp"),
        P(None, "dp", "tp"),
        P(None, "dp", "tp"),
        P(None, None, "tp"),
        P(None, "tp", None, None),
        P(None, "tp", None, None),
        P(None, "tp"),
        P(None, "tp", "dp"),
    )
    return jax.shard_map(
        functools.partial(per_device, physical(mesh)),
        mesh=mesh,
        in_specs=placed,
        out_specs=(P("tp", "dp"), P(None, "dp", "tp"), P(None, "dp", None, "tp")),
        check_vma=False,
    )
```

```python
import functools

import jax
import jax.numpy as jnp
from jax import lax
from jax.experimental import pallas as pl
from jax.experimental.pallas import tpu as pltpu
from jax.sharding import PartitionSpec as P

EPS = 1e-06
MESH = pl.DeviceIdType.MESH
LANES = 128
F32 = jnp.float32
BF16 = jnp.bfloat16


def partner(index, step, count):
    if count & (count - 1):
        raise ValueError(count)
    out = index
    bit = 1
    while bit < count:
        if step & bit:
            out = out + bit - 2 * bit * ((index // bit) % 2)
        bit *= 2
    return out


def pack_col(col):
    high = col.astype(BF16).astype(F32)
    low = col - high
    lane = lax.broadcasted_iota(jnp.int32, (col.shape[0], LANES), 1)
    return jnp.where(lane < LANES // 2, high, low).astype(BF16)


def unpack_col(lanes):
    return lanes[:, 0:1] + lanes[:, LANES // 2 : LANES // 2 + 1]


def step_kernel(
    sizes,
    stream_hbm, hidden_hbm, win_hbm, gain_hbm, path_hbm, gate_hbm, taps_hbm, rmap_hbm, imap_hbm, logit_hbm, outw_hbm,
    stream_out, hidden_out, window_out,
    xg, part, core_in, y_send, y_in, mix, upd, x_in, z_send, z_in,
    wpath, wgate, wout, hid, convp, rmap, imap, diag, win, gain, taps, logit,
    load_sem, load_small, load_once, ag_s, ag_r, fw_s, fw_r, b1_s, b1_r, b2_s, b2_r,
    c1_s, c1_r, c2_s, c2_r, d1_s, d1_r, d2_s, d2_r,
):
    layers, nz, nx, ny, nc, model = sizes
    tp = lax.axis_index("tp")
    dp = lax.axis_index("dp")
    z, x = tp // nx, tp % nx
    y, c = dp // nc, dp % nc
    rows, cols = stream_out.shape
    chans = wpath.shape[2]
    per_z = mix.shape[1] // nz
    chunk = mix.shape[2]

    def on_tp(zz, xx):
        return {"tp": zz * nx + xx, "dp": dp}

    def on_dp(yy, cc):
        return {"tp": tp, "dp": yy * nc + cc}

    loads = {}

    def load(name, layer, src, dst, sem):
        copy = pltpu.make_async_copy(src.at[layer], dst.at[layer], sem)
        copy.start()
        loads[name, layer] = copy

    peers = (
        [on_tp(partner(z, k, nz), x) for k in range(1, nz)]
        + [on_tp(z, partner(x, k, nx)) for k in range(1, nx)]
        + [on_dp(partner(y, k, ny), c) for k in range(1, ny)]
        + [on_dp(y, partner(c, k, nc)) for k in range(1, nc)]
    )
    barrier = pltpu.get_barrier_semaphore()
    for peer in peers:
        pl.semaphore_signal(barrier, inc=1, device_id=peer, device_id_type=MESH)
    once = [
        pltpu.make_async_copy(src, dst, load_once.at[at])
        for at, (src, dst) in enumerate(
            ((stream_hbm, xg.at[0, tp]), (gain_hbm, gain), (taps_hbm, taps), (logit_hbm, logit))
        )
    ]
    for copy in once:
        copy.start()
    load("path", 0, path_hbm, wpath, load_sem.at[0, 0])
    load("gate", 0, gate_hbm, wgate, load_sem.at[0, 1])
    for layer in range(layers):
        load("rmap", layer, rmap_hbm, rmap, load_small.at[layer, 0])
        load("imap", layer, imap_hbm, imap, load_small.at[layer, 1])
    once[0].wait()
    pl.semaphore_wait(barrier, len(peers))

    sends = []

    def send(src, dst, ssem, rsem, peer, cond=None):
        copy = pltpu.make_async_remote_copy(
            src_ref=src, dst_ref=dst, send_sem=ssem, recv_sem=rsem, device_id=peer, device_id_type=MESH
        )
        sends.append((copy, cond))
        if cond is None:
            copy.start()
        else:
            pl.when(cond)(copy.start)

    def arrived(dst, ssem, rsem, peer):
        pltpu.make_async_remote_copy(
            src_ref=dst, dst_ref=dst, send_sem=ssem, recv_sem=rsem, device_id=peer, device_id_type=MESH
        ).wait_recv()

    def gather_start(layer):
        own = xg.at[layer, tp]
        for k in range(1, nz):
            send(own, own, ag_s.at[layer, k], ag_r.at[layer, z], on_tp(partner(z, k, nz), x))
        for j in range(1, nx):
            send(own, own, fw_s.at[layer, nz, j], fw_r.at[layer, z, j], on_tp(z, partner(x, j, nx)))

    def project(layer, zz):
        block = xg[layer, pl.ds(zz * nx, nx)].reshape(nx * rows, cols).astype(F32)
        scaled = (block * gain[layer : layer + 1, :]).astype(BF16)
        square = jnp.sum(block * block, axis=1, keepdims=True)
        shape = (per_z, chunk)
        here = pl.ds(zz * per_z, per_z)
        part[layer, here, :, 0:chans] = (
            jnp.dot(scaled, wpath[layer], preferred_element_type=F32).astype(BF16).reshape(*shape, chans)
        )
        part[layer, here, :, chans : 2 * chans] = (
            jnp.dot(scaled, wgate[layer], preferred_element_type=F32).astype(BF16).reshape(*shape, chans)
        )
        part[layer, here, :, 2 * chans :] = pack_col(square).reshape(*shape, LANES)

    def forward(layer, zz):
        own = xg.at[layer, zz * nx + x]

        def wait():
            arrived(own, ag_s.at[layer, 0], ag_r.at[layer, zz], on_tp(partner(z, 1, nz), x))

        pl.when(zz != z)(wait)
        for j in range(1, nx):
            send(
                own, own, fw_s.at[layer, zz, j], fw_r.at[layer, zz, j], on_tp(z, partner(x, j, nx)), zz != z
            )

    def reduce_cores(layer, yy):
        both = part[layer, yy * nc + c].astype(F32)
        for j in range(1, nc):
            arrived(
                core_in.at[layer, j, yy], b1_s.at[layer, 0], b1_r.at[layer, j, yy], on_dp(y, partner(c, j, nc))
            )
            both = both + core_in[layer, j, yy].astype(F32)
        return both

    def gather_project_reduce(layer):
        each = nz // ny
        order = [
            (ky, partner(y, ky, ny) * each + partner(z % each, kl, each))
            for ky in list(range(1, ny)) + [0]
            for kl in range(each)
        ]
        forward(layer, order[0][1])
        for at, (ky, zz) in enumerate(order):
            if at + 1 < nz:
                forward(layer, order[at + 1][1])
            if at == 0:
                loads["path", layer].wait()
                loads["gate", layer].wait()
            for j in range(1, nx):
                xx = partner(x, j, nx)
                arrived(xg.at[layer, zz * nx + xx], fw_s.at[layer, nz, j], fw_r.at[layer, zz, j], on_tp(z, xx))
            project(layer, zz)
            for i in range(per_z):
                d = zz * per_z + i
                for j in range(1, nc):
                    cc = partner(c, j, nc)
                    send(
                        part.at[layer, d], core_in.at[layer, j, d // nc],
                        b1_s.at[layer, d], b1_r.at[layer, j, d // nc], on_dp(y, cc), d % nc == cc,
                    )
            if at % each == each - 1 and ky:
                yy = partner(y, ky, ny)
                both = reduce_cores(layer, yy)
                y_send[layer, ky, :, 0 : 2 * chans] = both[:, : 2 * chans].astype(BF16)
                y_send[layer, ky, :, 2 * chans :] = pack_col(unpack_col(both[:, 2 * chans :]))
                send(y_send.at[layer, ky], y_in.at[layer, ky], b2_s.at[layer, ky], b2_r.at[layer, ky], on_dp(yy, c))
        total = reduce_cores(layer, y)
        for k in range(1, ny):
            arrived(y_in.at[layer, k], b2_s.at[layer, k], b2_r.at[layer, k], on_dp(partner(y, k, ny), c))
            total = total + y_in[layer, k].astype(F32)
        return total

    def recur(layer, total):
        loads["hidden", layer].wait()
        scale = lax.rsqrt(unpack_col(total[:, 2 * chans :]) / model + EPS)
        zpath = (total[:, :chans] * scale).astype(BF16)
        zgate = (total[:, chans : 2 * chans] * scale).astype(BF16).astype(F32)
        window_out[layer, window_out.shape[1] - 1] = zpath
        last = taps.shape[1] - 1
        conv = convp[layer] + zpath.astype(F32) * taps[layer, last : last + 1, :]
        keep = jax.nn.log_sigmoid(logit[layer : layer + 1, :]) * 8.0
        gated = 0.5 * zgate * (1.0 + jnp.tanh(0.7978845608028654 * (zgate + 0.044715 * zgate * zgate * zgate)))
        wide = diag.shape[2]
        for p in range(diag.shape[1]):
            at = slice(p * wide, (p + 1) * wide)
            cb = conv[:, at]
            both = jnp.dot(cb, diag[layer, p], preferred_element_type=F32, precision=lax.Precision.HIGHEST)
            rgate = jax.nn.sigmoid(both[:, :wide])
            igate = jax.nn.sigmoid(both[:, wide:])
            loga = rgate * keep[:, at]
            decay = jnp.exp(loga)
            new = decay * hid[layer, :, at] + jnp.sqrt(-jnp.tanh(loga) * (1.0 + decay * decay)) * (igate * cb)
            hidden_out[layer, :, at] = new
            mix[layer, dp, :, at] = (new * gated[:, at]).astype(BF16)

    def share_and_emit(layer):
        own = mix.at[layer, dp]
        for k in range(1, ny):
            send(own, own, c1_s.at[layer, k], c1_r.at[layer, k], on_dp(partner(y, k, ny), c))
        for j in range(1, nc):
            send(own, own, c2_s.at[layer, 0, j], c2_r.at[layer, 0, j], on_dp(y, partner(c, j, nc)))
        loads["outw", layer].wait()
        if per_z == 1:
            emit(layer, dp)
        later = []
        for k in range(ny):
            yy = partner(y, k, ny)
            if k:
                theirs = mix.at[layer, yy * nc + c]
                arrived(theirs, c1_s.at[layer, k], c1_r.at[layer, k], on_dp(yy, c))
                for j in range(1, nc):
                    send(theirs, theirs, c2_s.at[layer, k, j], c2_r.at[layer, k, j], on_dp(y, partner(c, j, nc)))
                if per_z == 1:
                    emit(layer, yy * nc + c)
            for j in range(1, nc):
                cc = partner(c, j, nc)
                arrived(
                    mix.at[layer, yy * nc + cc], c2_s.at[layer, k, j], c2_r.at[layer, k, j], on_dp(y, cc)
                )
                if per_z == 1:
                    emit(layer, yy * nc + cc)
        if per_z != 1:
            for zz in range(nz):
                emit(layer, zz)

    def emit(layer, zz):
        block = mix[layer, pl.ds(zz * per_z, per_z)].reshape(per_z * chunk, chans)
        upd[layer, pl.ds(zz * nx, nx)] = (
            jnp.dot(block, wout[layer], preferred_element_type=F32).astype(BF16).reshape(nx, rows, cols)
        )
        for j in range(1, nx):
            xx = partner(x, j, nx)
            send(
                upd.at[layer, zz * nx + xx], x_in.at[layer, j, zz],
                d1_s.at[layer, j, zz], d1_r.at[layer, j, zz], on_tp(z, xx),
            )

    def reduce_stream(layer):
        if per_z == 1:
            order = [
                partner(y, ky, ny) * nc + partner(c, kc, nc) for ky in range(ny) for kc in range(nc)
            ]
        else:
            order = list(range(nz))
        for k, zz in enumerate(order):
            both = upd[layer, zz * nx + x].astype(F32)
            for j in range(1, nx):
                arrived(
                    x_in.at[layer, j, zz], d1_s.at[layer, j, zz], d1_r.at[layer, j, zz], on_tp(z, partner(x, j, nx))
                )
                both = both + x_in[layer, j, zz].astype(F32)
            z_send[layer, zz] = both.astype(BF16)
            send(
                z_send.at[layer, zz], z_in.at[layer, z], d2_s.at[layer, zz], d2_r.at[layer, z], on_tp(zz, x), zz != z
            )
        total = xg[layer, tp].astype(F32) + z_send[layer, z].astype(F32)
        for k in range(1, nz):
            zz = partner(z, k, nz)
            arrived(z_in.at[layer, zz], d2_s.at[layer, zz], d2_r.at[layer, zz], on_tp(zz, x))
            total = total + z_in[layer, zz].astype(F32)
        return total.astype(BF16)

    gather_start(0)
    for layer in range(layers):
        load("hidden", layer, hidden_hbm, hid, load_sem.at[layer, 2])
        load("window", layer, win_hbm, win, load_sem.at[layer, 3])
        load("outw", layer, outw_hbm, wout, load_sem.at[layer, 4])
        if layer:
            load("path", layer, path_hbm, wpath, load_sem.at[layer, 0])
            load("gate", layer, gate_hbm, wgate, load_sem.at[layer, 1])

    width = rmap.shape[2]
    row = lax.broadcasted_iota(jnp.int32, (width, 2 * width), 0)
    col = lax.broadcasted_iota(jnp.int32, (width, 2 * width), 1)
    place = [jnp.where(col == row + half * width, 1.0, 0.0).astype(F32) for half in range(2)]
    for layer in range(layers):
        loads["rmap", layer].wait()
        loads["imap", layer].wait()
        for p in range(diag.shape[1]):
            for half in range(2):
                for which, maps in enumerate((rmap, imap)):
                    diag[
                        layer, p, half * width : (half + 1) * width, which * 2 * width : (which + 1) * 2 * width
                    ] = jnp.dot(
                        maps[layer, 2 * p + half], place[half],
                        preferred_element_type=F32, precision=lax.Precision.HIGHEST,
                    )

    for copy in once[1:]:
        copy.wait()
    for layer in range(layers):
        loads["window", layer].wait()
        count = win.shape[1]
        convp[layer] = sum(win[layer, j].astype(F32) * taps[layer, j : j + 1, :] for j in range(count))
        for j in range(1, count):
            window_out[layer, j - 1] = win[layer, j]

    for layer in range(layers):
        recur(layer, gather_project_reduce(layer))
        share_and_emit(layer)
        new = reduce_stream(layer)
        if layer + 1 < layers:
            xg[layer + 1, tp] = new
            gather_start(layer + 1)
        else:
            stream_out[...] = new
    for copy, cond in sends:
        if cond is None:
            copy.wait_send()
        else:
            pl.when(cond)(copy.wait_send)


def per_device(
    grid,
    stream_in, hidden_state, window, norm_gain, path_weight, output_gate_weight,
    conv_taps, recur_map, input_map, decay_logit, out_weight,
):
    nz, nx, ny, nc = grid
    rows, cols = stream_in.shape
    layers, chunk, chans = hidden_state.shape
    tp, dp = nz * nx, ny * nc
    width = recur_map.shape[2]
    blocks = recur_map.shape[1]
    taps = conv_taps.shape[1]
    wide = 2 * chans + LANES
    vm = pl.BlockSpec(memory_space=pltpu.VMEM)
    hbm = pl.BlockSpec(memory_space=pltpu.HBM)
    dma = pltpu.SemaphoreType.DMA
    stream_out, hidden_next, window_next = pl.pallas_call(
        functools.partial(step_kernel, (layers, nz, nx, ny, nc, cols * dp)),
        out_shape=(
            jax.ShapeDtypeStruct((rows, cols), BF16),
            jax.ShapeDtypeStruct((layers, chunk, chans), F32),
            jax.ShapeDtypeStruct((layers, taps - 1, chunk, chans), BF16),
        ),
        in_specs=[hbm] * 11,
        out_specs=(vm, vm, vm),
        scratch_shapes=[
            pltpu.VMEM((layers, tp, rows, cols), BF16),
            pltpu.VMEM((layers, dp, chunk, wide), BF16),
            pltpu.VMEM((layers, nc, ny, chunk, wide), BF16),
            pltpu.VMEM((layers, ny, chunk, wide), BF16),
            pltpu.VMEM((layers, ny, chunk, wide), BF16),
            pltpu.VMEM((layers, dp, chunk, chans), BF16),
            pltpu.VMEM((layers, tp, rows, cols), BF16),
            pltpu.VMEM((layers, nx, nz, rows, cols), BF16),
            pltpu.VMEM((layers, nz, rows, cols), BF16),
            pltpu.VMEM((layers, nz, rows, cols), BF16),
            pltpu.VMEM((layers, cols, chans), BF16),
            pltpu.VMEM((layers, cols, chans), BF16),
            pltpu.VMEM((layers, chans, cols), BF16),
            pltpu.VMEM((layers, chunk, chans), F32),
            pltpu.VMEM((layers, chunk, chans), F32),
            pltpu.VMEM((layers, blocks, width, width), F32),
            pltpu.VMEM((layers, blocks, width, width), F32),
            pltpu.VMEM((layers, blocks // 2, 2 * width, 4 * width), F32),
            pltpu.VMEM((layers, taps - 1, chunk, chans), BF16),
            pltpu.VMEM((layers, cols), F32),
            pltpu.VMEM((layers, taps, chans), F32),
            pltpu.VMEM((layers, chans), F32),
            dma((layers, 5)), dma((layers, 2)), dma((4,)),
            dma((layers, nz)), dma((layers, nz)), dma((layers, nz + 1, nx)), dma((layers, nz, nx)),
            dma((layers, dp)), dma((layers, nc, ny)), dma((layers, ny)), dma((layers, ny)),
            dma((layers, ny)), dma((layers, ny)), dma((layers, ny, nc)), dma((layers, ny, nc)),
            dma((layers, nx, nz)), dma((layers, nx, nz)), dma((layers, nz)), dma((layers, nz)),
        ],
        compiler_params=pltpu.CompilerParams(
            collective_id=0, has_side_effects=True, vmem_limit_bytes=67043328
        ),
    )(
        stream_in, hidden_state, jnp.transpose(window, (0, 2, 1, 3)), norm_gain, path_weight, output_gate_weight,
        conv_taps, recur_map, input_map, decay_logit, out_weight,
    )
    return stream_out, hidden_next, jnp.transpose(window_next, (0, 2, 1, 3))


def physical(mesh):
    first = mesh.devices.flat[0]
    tp, dp = mesh.shape["tp"], mesh.shape["dp"]
    if getattr(first, "coords", None) is None:
        nx, nc = 2, 2
    else:
        nx = len({d.coords[0] for d in mesh.devices.flat})
        nc = len({d.core_on_chip for d in mesh.devices.flat})
    return tp // nx, nx, dp // nc, nc


def solution(mesh):
    placed = (
        P("tp", "dp"),
        P(None, "dp", "tp"),
        P(None, "dp", None, "tp"),
        P(None, "dp"),
        P(None, "dp", "tp"),
        P(None, "dp", "tp"),
        P(None, None, "tp"),
        P(None, "tp", None, None),
        P(None, "tp", None, None),
        P(None, "tp"),
        P(None, "tp", "dp"),
    )
    return jax.shard_map(
        functools.partial(per_device, physical(mesh)),
        mesh=mesh,
        in_specs=placed,
        out_specs=(P("tp", "dp"), P(None, "dp", "tp"), P(None, "dp", None, "tp")),
        check_vma=False,
    )
```
